32 devices in a mesh: tp: 32 (over z, y, x, core).
Axes of the slice: x: 2, y: 2, z: 4, core: 2. Of those that a mesh axis runs over, the one named last changes fastest.
Arguments:
- tokens: bfloat16 [32, 8, 4096], P('tp'), may hold values from -6 to 6
- block_norm_gain: float32 [2, 4096], replicated, may hold values from 0.1 to 1.9
- receptance_weight: bfloat16 [2, 32, 4096, 64], P(None, 'tp'), may hold values from -0.09375 to 0.09375
- key_weight: bfloat16 [2, 32, 4096, 64], P(None, 'tp'), may hold values from -0.09375 to 0.09375
- value_weight: bfloat16 [2, 32, 4096, 64], P(None, 'tp'), may hold values from -0.09375 to 0.09375
- decay_weight: bfloat16 [2, 32, 4096, 64], P(None, 'tp'), may hold values from -0.09375 to 0.09375
- learning_rate_weight: bfloat16 [2, 32, 4096, 64], P(None, 'tp'), may hold values from -0.09375 to 0.09375
- gate_weight: bfloat16 [2, 32, 4096, 64], P(None, 'tp'), may hold values from -0.09375 to 0.09375
- decay_bias_fixed: float32 [2, 2048], replicated, may hold values from -5 to 2
- self_token_weight: float32 [2, 2048], replicated, may hold values from -1.5 to 1.5
- readout_norm_gain: float32 [2, 2048], replicated, may hold values from 0.1 to 1.9
- output_weight: bfloat16 [2, 32, 64, 4096], P(None, 'tp'), may hold values from -0.125 to 0.125
- state: float32 [2, 32, 256, 4096], P(None, 'tp'), may hold values from -3 to 3
Outputs:
- mixed: bfloat16 [32, 8, 4096], P('tp')
- new_state: float32 [2, 32, 256, 4096], P(None, 'tp')
The draws below stay inside these ranges and needn't reach their ends.
All inputs are finite; a program needn't handle non-finite values.
Results may differ from the reference program's by a relative error of at most 0.018.
Values may be sent and summed in bfloat16 or wider, within the bound.
A program may use at most 128 MiB of HBM per device.

```python
import jax
import jax.numpy as jnp
from jax import lax

D = 4096
MIXER_WIDTH = 2048
HEAD_CHANNELS = 64
WINDOW_LAYERS = 2
SEQS = 256
MIXER_HEADS = 32
ROW_BLOCKS = 1
N_TP = 32


def shard_levels(own_key, shape, split, smallest, largest):
    gain = 1.0
    for axis_at, blocks in split:
        steps = jax.random.uniform(jax.random.fold_in(jax.random.fold_in(own_key, 6), axis_at), (blocks,), jnp.float32, smallest / len(split), largest / len(split))
        gain = gain * jnp.repeat(jnp.exp(steps), shape[axis_at] // blocks).reshape((-1,) + (1,) * (len(shape) - 1 - axis_at))
    return gain


def scatter_about(own_key, shape, width, most, pieces=(), dtype=jnp.bfloat16):
    loudness = shard_levels(own_key, shape, pieces, -0.22, 0.18) if pieces else 1.0
    entries = jax.random.normal(own_key, shape, jnp.float32) * width * loudness
    return jnp.minimum(jnp.maximum(entries, -most), most).astype(dtype)


def setup_inputs(seed: int = 0) -> dict:
    streams_of = jax.random.split(jax.random.key(seed), 14)
    tokens = scatter_about(streams_of[0], (N_TP, SEQS // MIXER_HEADS, D // ROW_BLOCKS), 1.0, 6.0, ((0, 32),))
    block_norm_gain = jnp.clip(1.0 + 0.18 * jax.random.normal(streams_of[1], (WINDOW_LAYERS, D), jnp.float32), 0.1, 1.9)
    receptance_weight = scatter_about(streams_of[2], (WINDOW_LAYERS, N_TP, D // ROW_BLOCKS, HEAD_CHANNELS), D ** -0.5, 0.09375, ((1, 32),))
    key_weight = scatter_about(streams_of[3], (WINDOW_LAYERS, N_TP, D // ROW_BLOCKS, HEAD_CHANNELS), D ** -0.5, 0.09375, ((1, 32),))
    value_weight = scatter_about(streams_of[4], (WINDOW_LAYERS, N_TP, D // ROW_BLOCKS, HEAD_CHANNELS), D ** -0.5, 0.09375, ((1, 32),))
    decay_weight = scatter_about(streams_of[5], (WINDOW_LAYERS, N_TP, D // ROW_BLOCKS, HEAD_CHANNELS), D ** -0.5, 0.09375, ((1, 32),))
    learning_rate_weight = scatter_about(streams_of[6], (WINDOW_LAYERS, N_TP, D // ROW_BLOCKS, HEAD_CHANNELS), D ** -0.5, 0.09375, ((1, 32),))
    gate_weight = scatter_about(streams_of[7], (WINDOW_LAYERS, N_TP, D // ROW_BLOCKS, HEAD_CHANNELS), D ** -0.5, 0.09375, ((1, 32),))
    decay_bias_fixed = jnp.clip(jax.random.uniform(streams_of[8], (WINDOW_LAYERS, MIXER_WIDTH), jnp.float32, -5.0, 2.0), -5.0, 2.0)
    self_token_weight = scatter_about(streams_of[9], (WINDOW_LAYERS, MIXER_WIDTH), 0.3, 1.5, (), jnp.float32)
    readout_norm_gain = jnp.clip(1.0 + 0.18 * jax.random.normal(streams_of[10], (WINDOW_LAYERS, MIXER_WIDTH), jnp.float32), 0.1, 1.9)
    output_weight = scatter_about(streams_of[11], (WINDOW_LAYERS, N_TP, HEAD_CHANNELS, D // ROW_BLOCKS), MIXER_WIDTH ** -0.5, 0.125, ((1, 32),))
    state = scatter_about(streams_of[12], (WINDOW_LAYERS, N_TP, SEQS // ROW_BLOCKS, HEAD_CHANNELS * HEAD_CHANNELS), 0.5, 3.0, ((1, 32),), jnp.float32)
    return {"tokens": tokens, "block_norm_gain": block_norm_gain, "receptance_weight": receptance_weight, "key_weight": key_weight, "value_weight": value_weight, "decay_weight": decay_weight, "learning_rate_weight": learning_rate_weight, "gate_weight": gate_weight, "decay_bias_fixed": decay_bias_fixed, "self_token_weight": self_token_weight, "readout_norm_gain": readout_norm_gain, "output_weight": output_weight, "state": state}


RMS_EPS = 1e-06
GROUP_EPS = 0.00064

def recurrent_update(layer_state, receptance_vector, key_vector, value_vector, decay_logits, learning_rate_logits, gate_logits, decay_constant, self_term_scale, head_gain_slice):
    highest = lax.Precision.HIGHEST
    shrink = jnp.exp(-jnp.exp(-jax.nn.softplus(-(decay_constant + decay_logits)) - 0.5))
    rate = jax.nn.sigmoid(learning_rate_logits)
    normed = key_vector * lax.rsqrt(lax.optimization_barrier(jnp.sum(key_vector * key_vector, -1, keepdims=True)) + 1.0)
    removed = jnp.einsum('...ij,...j->...i', layer_state, normed, precision=highest)
    layer_state = layer_state * shrink[..., None, :] - removed[..., :, None] * (normed * rate)[..., None, :] + value_vector[..., :, None] * (key_vector * rate)[..., None, :]
    readout = jnp.einsum('...ij,...j->...i', layer_state, receptance_vector, precision=highest)
    center = lax.optimization_barrier(jnp.mean(readout, -1, keepdims=True))
    spread = lax.optimization_barrier(jnp.mean(jnp.square(readout - center), -1, keepdims=True))
    normed_output = (readout - center) * lax.rsqrt(spread + GROUP_EPS) * head_gain_slice
    self_term = lax.optimization_barrier(jnp.sum(receptance_vector * key_vector * self_term_scale, -1, keepdims=True)) * value_vector
    return (((normed_output + self_term) * jax.nn.sigmoid(gate_logits)).astype(jnp.bfloat16), layer_state)

def reference(tokens, block_norm_gain, receptance_weight, key_weight, value_weight, decay_weight, learning_rate_weight, gate_weight, decay_bias_fixed, self_token_weight, readout_norm_gain, output_weight, state):
    seq_tile = SEQS // MIXER_HEADS
    col_tile = D // ROW_BLOCKS
    seq_block = SEQS // ROW_BLOCKS
    resid = tokens.reshape(MIXER_HEADS, ROW_BLOCKS, seq_tile, col_tile).transpose(0, 2, 1, 3).reshape(SEQS, D)

    def rows_full(weight):
        return weight.reshape(WINDOW_LAYERS, MIXER_HEADS, ROW_BLOCKS, col_tile, HEAD_CHANNELS).transpose(0, 2, 3, 1, 4).reshape(WINDOW_LAYERS, D, MIXER_WIDTH)
    fulls = [rows_full(weight) for weight in (receptance_weight, key_weight, value_weight, decay_weight, learning_rate_weight, gate_weight)]
    out_full = output_weight.reshape(WINDOW_LAYERS, MIXER_HEADS, ROW_BLOCKS, HEAD_CHANNELS, col_tile).transpose(0, 1, 3, 2, 4).reshape(WINDOW_LAYERS, MIXER_WIDTH, D)
    layer_states_stacked = state.reshape(WINDOW_LAYERS, MIXER_HEADS, ROW_BLOCKS, seq_block, HEAD_CHANNELS, HEAD_CHANNELS).transpose(0, 2, 3, 1, 4, 5)
    layer_states_stacked = layer_states_stacked.reshape(WINDOW_LAYERS, SEQS, MIXER_HEADS, HEAD_CHANNELS, HEAD_CHANNELS)
    updated = []
    for layer_index in range(WINDOW_LAYERS):
        wide = resid.astype(jnp.float32)
        scaled = (wide * block_norm_gain[layer_index]).astype(jnp.bfloat16)
        factor = lax.rsqrt(lax.optimization_barrier(jnp.mean(wide * wide, axis=1, keepdims=True)) + RMS_EPS)
        output_pieces = [(jnp.dot(scaled, full[layer_index], preferred_element_type=jnp.float32) * factor).reshape(SEQS, MIXER_HEADS, HEAD_CHANNELS) for full in fulls]
        head_results, layer_state = recurrent_update(layer_states_stacked[layer_index], *output_pieces, decay_bias_fixed[layer_index].reshape(MIXER_HEADS, HEAD_CHANNELS), self_token_weight[layer_index].reshape(MIXER_HEADS, HEAD_CHANNELS), readout_norm_gain[layer_index].reshape(MIXER_HEADS, HEAD_CHANNELS))
        branch = jnp.dot(head_results.reshape(SEQS, MIXER_WIDTH), out_full[layer_index], preferred_element_type=jnp.float32)
        resid = (wide + branch).astype(jnp.bfloat16)
        updated.append(layer_state)
    mixed = resid.reshape(MIXER_HEADS, seq_tile, ROW_BLOCKS, col_tile).transpose(0, 2, 1, 3).reshape(N_TP, seq_tile, col_tile)
    new_state = jnp.stack(updated).reshape(WINDOW_LAYERS, ROW_BLOCKS, seq_block, MIXER_HEADS, HEAD_CHANNELS, HEAD_CHANNELS).transpose(0, 3, 1, 2, 4, 5)
    new_state = new_state.reshape(WINDOW_LAYERS, N_TP, seq_block, HEAD_CHANNELS * HEAD_CHANNELS)
    return (mixed, new_state)
```

```python
import functools

import jax
import jax.numpy as jnp
from jax import lax
from jax.experimental import pallas as pl
from jax.experimental.pallas import tpu as pltpu
from jax.sharding import PartitionSpec as P

D = 4096


RMS_EPS = 1e-06
GROUP_EPS = 0.00064


def swapped(shard, axis, stride):
    return lax.ppermute(shard, axis, [(i, i ^ 1 << stride) for i in range(lax.axis_size(axis))])


def for_sending(shard):

    def short(part):
        return part.astype(jnp.bfloat16) if part.dtype == jnp.float32 else part

    return jax.tree.map(short, shard)


def recurrent_update(
    layer_state,
    receptance_vector,
    key_vector,
    value_vector,
    decay_logits,
    learning_rate_logits,
    gate_logits,
    decay_constant,
    self_term_scale,
    head_gain_slice,
):
    highest = lax.Precision.HIGHEST
    shrink = jnp.exp(-jnp.exp(-jax.nn.softplus(-(decay_constant + decay_logits)) - 0.5))
    rate = jax.nn.sigmoid(learning_rate_logits)
    normed = key_vector * lax.rsqrt(jnp.sum(key_vector * key_vector, -1, keepdims=True) + 1.0)
    removed = jnp.einsum("...ij,...j->...i", layer_state, normed, precision=highest)
    layer_state = (
        layer_state * shrink[..., None, :]
        - removed[..., :, None] * (normed * rate)[..., None, :]
        + value_vector[..., :, None] * (key_vector * rate)[..., None, :]
    )
    readout = jnp.einsum("...ij,...j->...i", layer_state, receptance_vector, precision=highest)
    center = jnp.mean(readout, -1, keepdims=True)
    spread = jnp.mean(jnp.square(readout - center), -1, keepdims=True)
    normed_output = (readout - center) * lax.rsqrt(spread + GROUP_EPS) * head_gain_slice
    self_term = (
        jnp.sum(receptance_vector * key_vector * self_term_scale, -1, keepdims=True) * value_vector
    )
    return (
        ((normed_output + self_term) * jax.nn.sigmoid(gate_logits)).astype(jnp.bfloat16),
        layer_state,
    )


def double_gather(piece, position, first_bit, count, mover):
    for offset in range(count):
        which_bit = first_bit + offset
        partner = mover(piece, which_bit)
        lower_self = position >> which_bit & 1 == 0
        piece = jnp.where(
            lower_self, jnp.concatenate([piece, partner], 0), jnp.concatenate([partner, piece], 0)
        )
    return piece


def halve_sum(members, position, first_bit, count, mover):
    for offset in reversed(range(count)):
        which_bit = first_bit + offset
        upper_self = position >> which_bit & 1 == 1
        sends = tuple(
            (
                jnp.where(
                    upper_self, member[: member.shape[0] // 2], member[member.shape[0] // 2 :]
                )
                for member in members
            )
        )
        keeps = tuple(
            (
                jnp.where(
                    upper_self, member[member.shape[0] // 2 :], member[: member.shape[0] // 2]
                )
                for member in members
            )
        )
        arrived = mover(sends, which_bit)
        members = tuple((kept + got for kept, got in zip(keeps, arrived)))
    return members


def on_device(
    tokens,
    block_norm_gain,
    receptance_weight,
    key_weight,
    value_weight,
    decay_weight,
    learning_rate_weight,
    gate_weight,
    decay_bias_fixed,
    self_token_weight,
    readout_norm_gain,
    output_weight,
    state,
):
    columns_dev = tokens.shape[2]
    row_blocks = D // columns_dev
    low_bits = row_blocks.bit_length() - 1
    head_count = lax.axis_size("tp") // row_blocks
    high_bits = head_count.bit_length() - 1
    position = lax.axis_index("tp")
    head_index = position // row_blocks
    row_block = position % row_blocks
    head_size = receptance_weight.shape[3]
    seq_tile = tokens.shape[1]
    move_rows = lambda payload, which_bit: swapped(payload, "tp", which_bit)
    move_proj = lambda payload, which_bit: swapped(payload, "tp", which_bit)
    move_outs = lambda payload, which_bit: jax.tree.map(
        lambda part, own: part.astype(own.dtype),
        swapped(for_sending(payload), "tp", which_bit),
        payload,
    )
    move_split = lambda payload, which_bit: jax.tree.map(
        lambda part, own: part.astype(own.dtype),
        swapped(for_sending(payload), "tp", which_bit),
        payload,
    )

    def mixer(columns, layer_index):
        gain_cols = lax.dynamic_slice_in_dim(
            block_norm_gain[layer_index], row_block * columns_dev, columns_dev
        )
        wide = columns.astype(jnp.float32)
        scaled = (wide * gain_cols).astype(jnp.bfloat16)
        squares = jnp.sum(wide * wide, axis=1)
        weights = jnp.concatenate(
            [
                receptance_weight[layer_index, 0],
                key_weight[layer_index, 0],
                value_weight[layer_index, 0],
                decay_weight[layer_index, 0],
                learning_rate_weight[layer_index, 0],
                gate_weight[layer_index, 0],
            ],
            axis=1,
        )
        partial_value = jnp.dot(scaled, weights, preferred_element_type=jnp.float32)
        summed, total_sq = halve_sum((partial_value, squares), position, 0, low_bits, move_proj)
        projected = summed * lax.rsqrt(total_sq / D + RMS_EPS)[:, None]
        output_pieces = jnp.split(projected, 6, axis=1)

        def head_columns(table):
            return lax.dynamic_slice_in_dim(table[layer_index], head_index * head_size, head_size)

        layer_state = state[layer_index, 0].reshape(-1, head_size, head_size)
        out_tile, layer_state = recurrent_update(
            layer_state,
            *output_pieces,
            head_columns(decay_bias_fixed),
            head_columns(self_token_weight),
            head_columns(readout_norm_gain)
        )
        out_all = double_gather(out_tile, position, 0, low_bits, move_outs)
        branch = jnp.dot(out_all, output_weight[layer_index, 0], preferred_element_type=jnp.float32)
        return (branch, layer_state.reshape(layer_state.shape[0], head_size * head_size))

    columns = double_gather(tokens[0], position, low_bits, high_bits, move_rows)
    first_branch, first_memory = mixer(columns, 0)
    (tile_sum,) = halve_sum((first_branch,), position, low_bits, high_bits, move_split)
    tile_one = (tokens[0].astype(jnp.float32) + tile_sum).astype(jnp.bfloat16)
    columns = double_gather(tile_one, position, low_bits, high_bits, move_rows)
    second_branch, second_memory = mixer(columns, 1)
    (tile_sum,) = halve_sum((second_branch,), position, low_bits, high_bits, move_split)
    resid_rows = lax.dynamic_slice_in_dim(columns, head_index * seq_tile, seq_tile, 0)
    mixed = (resid_rows.astype(jnp.float32) + tile_sum).astype(jnp.bfloat16)
    new_state = jnp.stack([first_memory, second_memory])[:, None]
    return (mixed[None], new_state)


class Place:
    def __init__(self, n):
        me = lax.axis_index("tp")
        self.n, self.planes = n, n // 8
        self.me = me
        self.c = me % 2
        self.x = (me // 2) % 2
        self.y = (me // 4) % 2
        self.z = me // 8
        self.sib = me + 1 - 2 * self.c
        self.xn = me + 2 * (1 - 2 * self.x)
        self.yn = me + 4 * (1 - 2 * self.y)
        self.far = [self.planes // 2] + [k for k in range(1, self.planes) if k != self.planes // 2]
        self.near = [k for k in self.far if k != self.planes // 2] + [self.planes // 2]

    def plane(self, k):
        return (self.z + k) % self.planes

    def zn(self, k):
        return self.plane(k) * 8 + self.me % 8

    def greet(self):
        barrier = pltpu.get_barrier_semaphore()
        others = [self.sib, self.xn, self.yn] + [self.zn(k) for k in self.far]
        for other in others:
            pl.semaphore_signal(
                barrier, inc=1, device_id=(other,), device_id_type=pl.DeviceIdType.MESH
            )
        pl.semaphore_wait(barrier, len(others))


def remote(src, dst, send, recv, to):
    return pltpu.make_async_remote_copy(
        src_ref=src,
        dst_ref=dst,
        send_sem=send,
        recv_sem=recv,
        device_id=(to,),
        device_id_type=pl.DeviceIdType.MESH,
    )


def gather_sends(n):
    planes = n // 8
    return (planes - 1) + 3 * planes + 4 * planes + 2 * planes


def gather_phase(at, own_ref, full_ref, send, recv_a, recv_b):
    half = own_ref.shape[1] // 2
    first, second = pl.ds(0, half), pl.ds(half, half)
    started = []

    def tile(p, y, x, c):
        return ((p * 2 + y) * 2 + x) * 2 + c

    def go(src, t, to, cols=None, recv=recv_a):
        dst = full_ref.at[t]
        if cols is not None:
            src, dst = src.at[:, cols], dst.at[:, cols]
        copy = remote(src, dst, send.at[len(started)], recv.at[t], to)
        copy.start()
        started.append(copy)

    def arrived(t, cols=None, recv=recv_a):
        dst = full_ref.at[t]
        if cols is not None:
            dst = dst.at[:, cols]
        remote(dst, dst, send.at[0], recv.at[t], at.sib).wait_recv()

    for k in at.near:
        go(own_ref, at.me, at.zn(k))
    go(own_ref, at.me, at.xn)
    go(own_ref, at.me, at.yn)
    go(own_ref, at.me, at.sib)
    full_ref[at.me] = own_ref[...]

    def spread(k):
        p = at.plane(k)
        t = tile(p, at.y, 1 - at.x, at.c)
        arrived(t)
        go(full_ref.at[t], t, at.yn, first, recv_a)
        go(full_ref.at[t], t, at.sib)
        t = tile(p, 1 - at.y, at.x, at.c)
        arrived(t)
        go(full_ref.at[t], t, at.xn, second, recv_b)
        go(full_ref.at[t], t, at.sib)

    def corner(k):
        t = tile(at.plane(k), 1 - at.y, 1 - at.x, at.c)
        arrived(t, first, recv_a)
        go(full_ref.at[t], t, at.sib, first, recv_a)
        arrived(t, second, recv_b)
        go(full_ref.at[t], t, at.sib, second, recv_b)

    order = [0] + at.near
    for step, k in enumerate(order):
        if step:
            t = at.zn(k)
            arrived(t)
            go(full_ref.at[t], t, at.xn)
            go(full_ref.at[t], t, at.yn)
            go(full_ref.at[t], t, at.sib)
        if step >= 1:
            spread(order[step - 1])
        if step >= 2:
            corner(order[step - 2])
    spread(order[-1])
    if len(order) > 1:
        corner(order[-2])
    corner(order[-1])
    for k in order:
        p = at.plane(k)
        for y in (at.y, 1 - at.y):
            for x in (at.x, 1 - at.x):
                t = tile(p, y, x, 1 - at.c)
                if y is not at.y and x is not at.x:
                    arrived(t, first, recv_a)
                    arrived(t, second, recv_b)
                else:
                    arrived(t)
    for copy in started:
        copy.wait_send()


def gather_kernel(n, own_ref, full_ref, send, recv_a, recv_b):
    at = Place(n)
    at.greet()
    gather_phase(at, own_ref, full_ref, send, recv_a, recv_b)


def sum_scratch(n, rows, columns):
    planes, half = n // 8, columns // 2
    tiles = lambda count, width: pltpu.VMEM((count, rows, width), jnp.bfloat16)
    return [
        tiles(n // 2, columns),
        tiles(n // 2, columns),
        tiles(planes, half),
        tiles(planes, half),
        tiles(planes, columns),
        tiles(planes, columns),
        tiles(planes, columns),
        tiles(planes, columns),
        pltpu.SemaphoreType.DMA((6 * planes,)),
        pltpu.SemaphoreType.DMA((6 * planes,)),
    ]


def sum_phase(at, part_ref, scratch):
    sib, acc, in_a, in_b, in_x, in_y, out_z, in_z, send, recv = scratch
    planes = at.planes
    half = part_ref.shape[3] // 2
    first, second = pl.ds(0, half), pl.ds(half, half)
    order = at.far + [0]
    started = []

    def go(src, dst, kind, k, to):
        copy = remote(src, dst, send.at[kind * planes + k], recv.at[kind * planes + k], to)
        copy.start()
        started.append(copy)

    def arrived(dst, kind, k):
        slot = kind * planes + k
        remote(dst, dst, send.at[slot], recv.at[slot], at.sib).wait_recv()

    def f32(v):
        return v.astype(jnp.float32)

    def chunk(p, y, x):
        return (p * 2 + y) * 2 + x

    for k in order:
        block = pl.ds(at.plane(k) * 4, 4)
        go(part_ref.at[block, 1 - at.c], sib.at[block], 0, k, at.sib)
    for k in order:
        p = at.plane(k)
        block = pl.ds(p * 4, 4)
        arrived(sib.at[block], 0, k)
        for y, x in ((1 - at.y, 1 - at.x), (at.y, 1 - at.x), (1 - at.y, at.x), (at.y, at.x)):
            q = chunk(p, y, x)
            acc[q] = (f32(part_ref[q, at.c]) + f32(sib[q])).astype(jnp.bfloat16)
            if y is not at.y and x is not at.x:
                go(acc.at[q, :, first], in_a.at[k], 1, k, at.yn)
                go(acc.at[q, :, second], in_b.at[k], 2, k, at.xn)
    for k in order:
        p = at.plane(k)
        q = chunk(p, at.y, 1 - at.x)
        arrived(in_a.at[k], 1, k)
        acc[q, :, first] = (f32(acc[q, :, first]) + f32(in_a[k])).astype(jnp.bfloat16)
        go(acc.at[q], in_x.at[k], 3, k, at.xn)
        q = chunk(p, 1 - at.y, at.x)
        arrived(in_b.at[k], 2, k)
        acc[q, :, second] = (f32(acc[q, :, second]) + f32(in_b[k])).astype(jnp.bfloat16)
        go(acc.at[q], in_y.at[k], 4, k, at.yn)
    total = None
    for k in order:
        arrived(in_x.at[k], 3, k)
        arrived(in_y.at[k], 4, k)
        plane = f32(acc[chunk(at.plane(k), at.y, at.x)]) + f32(in_x[k]) + f32(in_y[k])
        if k:
            out_z[k] = plane.astype(jnp.bfloat16)
            go(out_z.at[k], in_z.at[k], 5, k, at.zn(k))
        else:
            total = plane
    for k in at.near:
        arrived(in_z.at[k], 5, k)
        total = total + f32(in_z[k])
    for copy in started:
        copy.wait_send()
    return total


def middle_kernel(n, part_ref, own_ref, full_ref, next_ref, *scratch):
    at = Place(n)
    at.greet()
    total = sum_phase(at, part_ref, scratch[:10])
    next_ref[...] = (own_ref[...].astype(jnp.float32) + total).astype(jnp.bfloat16)
    gather_phase(at, next_ref, full_ref, *scratch[10:])


def last_kernel(n, part_ref, own_ref, next_ref, *scratch):
    at = Place(n)
    at.greet()
    total = sum_phase(at, part_ref, scratch)
    next_ref[...] = (own_ref[...].astype(jnp.float32) + total).astype(jnp.bfloat16)


def comm_call(kernel, n, collective_id, out_shape, scratch_shapes, *operands):
    vmem = pl.BlockSpec(memory_space=pltpu.VMEM)
    return pl.pallas_call(
        functools.partial(kernel, n),
        out_shape=out_shape,
        in_specs=[vmem] * len(operands),
        out_specs=jax.tree.map(lambda _: vmem, out_shape),
        scratch_shapes=scratch_shapes,
        compiler_params=pltpu.CompilerParams(
            collective_id=collective_id, has_side_effects=True, vmem_limit_bytes=40 << 20
        ),
    )(*operands)


def gather_scratch(n):
    return [
        pltpu.SemaphoreType.DMA((gather_sends(n),)),
        pltpu.SemaphoreType.DMA((n,)),
        pltpu.SemaphoreType.DMA((n,)),
    ]


def on_device_fast(n, *args):
    tokens, gain, wr, wk, wv, wd, wq, wg, bias, self_w, ro_gain, w_out, state = args
    own = tokens[0]
    rows, columns = own.shape
    head = wr.shape[3]
    full_shape = jax.ShapeDtypeStruct((n, rows, columns), own.dtype)
    own_shape = jax.ShapeDtypeStruct(own.shape, own.dtype)
    position = lax.axis_index("tp")
    new_state = []

    def mixer(full, layer):
        x = full.reshape(n * rows, columns)
        wide = x.astype(jnp.float32)
        scaled = (wide * gain[layer]).astype(jnp.bfloat16)
        inv = lax.rsqrt(jnp.mean(wide * wide, axis=1) + RMS_EPS)[:, None]
        pieces = [
            jnp.dot(scaled, w[layer, 0], preferred_element_type=jnp.float32) * inv
            for w in (wr, wk, wv, wd, wq, wg)
        ]
        cols = lambda table: lax.dynamic_slice_in_dim(table[layer], position * head, head)
        o, s = recurrent_update(
            state[layer, 0].reshape(-1, head, head), *pieces, cols(bias), cols(self_w), cols(ro_gain)
        )
        new_state.append(s.reshape(s.shape[0], head * head))
        part = jnp.dot(o, w_out[layer, 0], preferred_element_type=jnp.float32)
        return part.astype(jnp.bfloat16).reshape(n // 2, 2, rows, columns)

    full = comm_call(gather_kernel, n, 0, full_shape, gather_scratch(n), own)
    part = mixer(full, 0)
    full, own = comm_call(
        middle_kernel,
        n,
        1,
        (full_shape, own_shape),
        sum_scratch(n, rows, columns) + gather_scratch(n),
        part,
        own,
    )
    part = mixer(full, 1)
    mixed = comm_call(last_kernel, n, 2, own_shape, sum_scratch(n, rows, columns), part, own)
    return mixed[None], jnp.stack(new_state)[:, None]


def pick(n, *args):
    one_block = args[0].shape[2] == args[1].shape[1]
    if one_block and n % 16 == 0:
        return on_device_fast(n, *args)
    return on_device(*args)


def solution(mesh):
    return jax.shard_map(
        functools.partial(pick, mesh.shape["tp"]),
        mesh=mesh,
        in_specs=(
            P("tp", None, None),
            P(),
            P(None, "tp", None, None),
            P(None, "tp", None, None),
            P(None, "tp", None, None),
            P(None, "tp", None, None),
            P(None, "tp", None, None),
            P(None, "tp", None, None),
            P(),
            P(),
            P(),
            P(None, "tp", None, None),
            P(None, "tp", None, None),
        ),
        out_specs=(P("tp", None, None), P(None, "tp", None, None)),
        check_vma=False,
    )
```

```python
import functools

import jax
import jax.numpy as jnp
from jax import lax
from jax.experimental import pallas as pl
from jax.experimental.pallas import tpu as pltpu
from jax.sharding import PartitionSpec as P

D = 4096


RMS_EPS = 1e-06
GROUP_EPS = 0.00064


def swapped(shard, axis, stride):
    return lax.ppermute(shard, axis, [(i, i ^ 1 << stride) for i in range(lax.axis_size(axis))])


def for_sending(shard):

    def short(part):
        return part.astype(jnp.bfloat16) if part.dtype == jnp.float32 else part

    return jax.tree.map(short, shard)


def recurrent_update(
    layer_state,
    receptance_vector,
    key_vector,
    value_vector,
    decay_logits,
    learning_rate_logits,
    gate_logits,
    decay_constant,
    self_term_scale,
    head_gain_slice,
):
    highest = lax.Precision.HIGHEST
    shrink = jnp.exp(-jnp.exp(-jax.nn.softplus(-(decay_constant + decay_logits)) - 0.5))
    rate = jax.nn.sigmoid(learning_rate_logits)
    normed = key_vector * lax.rsqrt(jnp.sum(key_vector * key_vector, -1, keepdims=True) + 1.0)
    removed = jnp.einsum("...ij,...j->...i", layer_state, normed, precision=highest)
    layer_state = (
        layer_state * shrink[..., None, :]
        - removed[..., :, None] * (normed * rate)[..., None, :]
        + value_vector[..., :, None] * (key_vector * rate)[..., None, :]
    )
    readout = jnp.einsum("...ij,...j->...i", layer_state, receptance_vector, precision=highest)
    center = jnp.mean(readout, -1, keepdims=True)
    spread = jnp.mean(jnp.square(readout - center), -1, keepdims=True)
    normed_output = (readout - center) * lax.rsqrt(spread + GROUP_EPS) * head_gain_slice
    self_term = (
        jnp.sum(receptance_vector * key_vector * self_term_scale, -1, keepdims=True) * value_vector
    )
    return (
        ((normed_output + self_term) * jax.nn.sigmoid(gate_logits)).astype(jnp.bfloat16),
        layer_state,
    )


def double_gather(piece, position, first_bit, count, mover):
    for offset in range(count):
        which_bit = first_bit + offset
        partner = mover(piece, which_bit)
        lower_self = position >> which_bit & 1 == 0
        piece = jnp.where(
            lower_self, jnp.concatenate([piece, partner], 0), jnp.concatenate([partner, piece], 0)
        )
    return piece


def halve_sum(members, position, first_bit, count, mover):
    for offset in reversed(range(count)):
        which_bit = first_bit + offset
        upper_self = position >> which_bit & 1 == 1
        sends = tuple(
            (
                jnp.where(
                    upper_self, member[: member.shape[0] // 2], member[member.shape[0] // 2 :]
                )
                for member in members
            )
        )
        keeps = tuple(
            (
                jnp.where(
                    upper_self, member[member.shape[0] // 2 :], member[: member.shape[0] // 2]
                )
                for member in members
            )
        )
        arrived = mover(sends, which_bit)
        members = tuple((kept + got for kept, got in zip(keeps, arrived)))
    return members


def on_device(
    tokens,
    block_norm_gain,
    receptance_weight,
    key_weight,
    value_weight,
    decay_weight,
    learning_rate_weight,
    gate_weight,
    decay_bias_fixed,
    self_token_weight,
    readout_norm_gain,
    output_weight,
    state,
):
    columns_dev = tokens.shape[2]
    row_blocks = D // columns_dev
    low_bits = row_blocks.bit_length() - 1
    head_count = lax.axis_size("tp") // row_blocks
    high_bits = head_count.bit_length() - 1
    position = lax.axis_index("tp")
    head_index = position // row_blocks
    row_block = position % row_blocks
    head_size = receptance_weight.shape[3]
    seq_tile = tokens.shape[1]
    move_rows = lambda payload, which_bit: swapped(payload, "tp", which_bit)
    move_proj = lambda payload, which_bit: swapped(payload, "tp", which_bit)
    move_outs = lambda payload, which_bit: jax.tree.map(
        lambda part, own: part.astype(own.dtype),
        swapped(for_sending(payload), "tp", which_bit),
        payload,
    )
    move_split = lambda payload, which_bit: jax.tree.map(
        lambda part, own: part.astype(own.dtype),
        swapped(for_sending(payload), "tp", which_bit),
        payload,
    )

    def mixer(columns, layer_index):
        gain_cols = lax.dynamic_slice_in_dim(
            block_norm_gain[layer_index], row_block * columns_dev, columns_dev
        )
        wide = columns.astype(jnp.float32)
        scaled = (wide * gain_cols).astype(jnp.bfloat16)
        squares = jnp.sum(wide * wide, axis=1)
        weights = jnp.concatenate(
            [
                receptance_weight[layer_index, 0],
                key_weight[layer_index, 0],
                value_weight[layer_index, 0],
                decay_weight[layer_index, 0],
                learning_rate_weight[layer_index, 0],
                gate_weight[layer_index, 0],
            ],
            axis=1,
        )
        partial_value = jnp.dot(scaled, weights, preferred_element_type=jnp.float32)
        summed, total_sq = halve_sum((partial_value, squares), position, 0, low_bits, move_proj)
        projected = summed * lax.rsqrt(total_sq / D + RMS_EPS)[:, None]
        output_pieces = jnp.split(projected, 6, axis=1)

        def head_columns(table):
            return lax.dynamic_slice_in_dim(table[layer_index], head_index * head_size, head_size)

        layer_state = state[layer_index, 0].reshape(-1, head_size, head_size)
        out_tile, layer_state = recurrent_update(
            layer_state,
            *output_pieces,
            head_columns(decay_bias_fixed),
            head_columns(self_token_weight),
            head_columns(readout_norm_gain)
        )
        out_all = double_gather(out_tile, position, 0, low_bits, move_outs)
        branch = jnp.dot(out_all, output_weight[layer_index, 0], preferred_element_type=jnp.float32)
        return (branch, layer_state.reshape(layer_state.shape[0], head_size * head_size))

    columns = double_gather(tokens[0], position, low_bits, high_bits, move_rows)
    first_branch, first_memory = mixer(columns, 0)
    (tile_sum,) = halve_sum((first_branch,), position, low_bits, high_bits, move_split)
    tile_one = (tokens[0].astype(jnp.float32) + tile_sum).astype(jnp.bfloat16)
    columns = double_gather(tile_one, position, low_bits, high_bits, move_rows)
    second_branch, second_memory = mixer(columns, 1)
    (tile_sum,) = halve_sum((second_branch,), position, low_bits, high_bits, move_split)
    resid_rows = lax.dynamic_slice_in_dim(columns, head_index * seq_tile, seq_tile, 0)
    mixed = (resid_rows.astype(jnp.float32) + tile_sum).astype(jnp.bfloat16)
    new_state = jnp.stack([first_memory, second_memory])[:, None]
    return (mixed[None], new_state)


class Place:
    def __init__(self, n):
        me = lax.axis_index("tp")
        self.n, self.planes = n, n // 8
        self.me = me
        self.c = me % 2
        self.x = (me // 2) % 2
        self.y = (me // 4) % 2
        self.z = me // 8
        self.sib = me + 1 - 2 * self.c
        self.xn = me + 2 * (1 - 2 * self.x)
        self.yn = me + 4 * (1 - 2 * self.y)
        self.far = [self.planes // 2] + [k for k in range(1, self.planes) if k != self.planes // 2]
        self.near = [k for k in self.far if k != self.planes // 2] + [self.planes // 2]

    def plane(self, k):
        return (self.z + k) % self.planes

    def zn(self, k):
        return self.plane(k) * 8 + self.me % 8

    def greet(self):
        barrier = pltpu.get_barrier_semaphore()
        others = [self.sib, self.xn, self.yn] + [self.zn(k) for k in self.far]
        for other in others:
            pl.semaphore_signal(
                barrier, inc=1, device_id=(other,), device_id_type=pl.DeviceIdType.MESH
            )
        pl.semaphore_wait(barrier, len(others))


def remote(src, dst, send, recv, to):
    return pltpu.make_async_remote_copy(
        src_ref=src,
        dst_ref=dst,
        send_sem=send,
        recv_sem=recv,
        device_id=(to,),
        device_id_type=pl.DeviceIdType.MESH,
    )


def gather_sends(n):
    planes = n // 8
    return (planes - 1) + 3 * planes + 4 * planes + 2 * planes


def gather_phase(at, own_ref, full_ref, send, recv_a, recv_b):
    half = own_ref.shape[1] // 2
    first, second = pl.ds(0, half), pl.ds(half, half)
    started = []

    def tile(p, y, x, c):
        return ((p * 2 + y) * 2 + x) * 2 + c

    def go(src, t, to, cols=None, recv=recv_a):
        dst = full_ref.at[t]
        if cols is not None:
            src, dst = src.at[:, cols], dst.at[:, cols]
        copy = remote(src, dst, send.at[len(started)], recv.at[t], to)
        copy.start()
        started.append(copy)

    def arrived(t, cols=None, recv=recv_a):
        dst = full_ref.at[t]
        if cols is not None:
            dst = dst.at[:, cols]
        remote(dst, dst, send.at[0], recv.at[t], at.sib).wait_recv()

    for k in at.near:
        go(own_ref, at.me, at.zn(k))
    go(own_ref, at.me, at.xn)
    go(own_ref, at.me, at.yn)
    go(own_ref, at.me, at.sib)
    full_ref[at.me] = own_ref[...]

    def spread(k):
        p = at.plane(k)
        t = tile(p, at.y, 1 - at.x, at.c)
        arrived(t)
        go(full_ref.at[t], t, at.yn, first, recv_a)
        go(full_ref.at[t], t, at.sib)
        t = tile(p, 1 - at.y, at.x, at.c)
        arrived(t)
        go(full_ref.at[t], t, at.xn, second, recv_b)
        go(full_ref.at[t], t, at.sib)

    def corner(k):
        t = tile(at.plane(k), 1 - at.y, 1 - at.x, at.c)
        arrived(t, first, recv_a)
        go(full_ref.at[t], t, at.sib, first, recv_a)
        arrived(t, second, recv_b)
        go(full_ref.at[t], t, at.sib, second, recv_b)

    order = [0] + at.near
    for step, k in enumerate(order):
        if step:
            t = at.zn(k)
            arrived(t)
            go(full_ref.at[t], t, at.xn)
            go(full_ref.at[t], t, at.yn)
            go(full_ref.at[t], t, at.sib)
        if step >= 1:
            spread(order[step - 1])
        if step >= 2:
            corner(order[step - 2])
    spread(order[-1])
    if len(order) > 1:
        corner(order[-2])
    corner(order[-1])
    for k in order:
        p = at.plane(k)
        for y in (at.y, 1 - at.y):
            for x in (at.x, 1 - at.x):
                t = tile(p, y, x, 1 - at.c)
                if y is not at.y and x is not at.x:
                    arrived(t, first, recv_a)
                    arrived(t, second, recv_b)
                else:
                    arrived(t)
    for copy in started:
        copy.wait_send()


def gather_kernel(n, own_ref, full_ref, send, recv_a, recv_b):
    at = Place(n)
    at.greet()
    gather_phase(at, own_ref, full_ref, send, recv_a, recv_b)


def sum_scratch(n, rows, columns):
    planes, half = n // 8, columns // 2
    tiles = lambda count, width: pltpu.VMEM((count, rows, width), jnp.bfloat16)
    return [
        tiles(n // 2, columns),
        tiles(n // 2, columns),
        tiles(planes, half),
        tiles(planes, half),
        tiles(planes, columns),
        tiles(planes, columns),
        tiles(planes, columns),
        tiles(planes, columns),
        pltpu.SemaphoreType.DMA((6 * planes,)),
        pltpu.SemaphoreType.DMA((6 * planes,)),
    ]


def sum_phase(at, part_ref, scratch):
    sib, acc, in_a, in_b, in_x, in_y, out_z, in_z, send, recv = scratch
    planes = at.planes
    half = part_ref.shape[3] // 2
    first, second = pl.ds(0, half), pl.ds(half, half)
    order = at.far + [0]
    started = []

    def go(src, dst, kind, k, to):
        copy = remote(src, dst, send.at[kind * planes + k], recv.at[kind * planes + k], to)
        copy.start()
        started.append(copy)

    def arrived(dst, kind, k):
        slot = kind * planes + k
        remote(dst, dst, send.at[slot], recv.at[slot], at.sib).wait_recv()

    def f32(v):
        return v.astype(jnp.float32)

    def chunk(p, y, x):
        return (p * 2 + y) * 2 + x

    for k in order:
        block = pl.ds(at.plane(k) * 4, 4)
        go(part_ref.at[block, 1 - at.c], sib.at[block], 0, k, at.sib)
    for k in order:
        p = at.plane(k)
        block = pl.ds(p * 4, 4)
        arrived(sib.at[block], 0, k)
        for y, x in ((1 - at.y, 1 - at.x), (at.y, 1 - at.x), (1 - at.y, at.x), (at.y, at.x)):
            q = chunk(p, y, x)
            acc[q] = (f32(part_ref[q, at.c]) + f32(sib[q])).astype(jnp.bfloat16)
            if y is not at.y and x is not at.x:
                go(acc.at[q, :, first], in_a.at[k], 1, k, at.yn)
                go(acc.at[q, :, second], in_b.at[k], 2, k, at.xn)
    for k in order:
        p = at.plane(k)
        q = chunk(p, at.y, 1 - at.x)
        arrived(in_a.at[k], 1, k)
        acc[q, :, first] = (f32(acc[q, :, first]) + f32(in_a[k])).astype(jnp.bfloat16)
        go(acc.at[q], in_x.at[k], 3, k, at.xn)
        q = chunk(p, 1 - at.y, at.x)
        arrived(in_b.at[k], 2, k)
        acc[q, :, second] = (f32(acc[q, :, second]) + f32(in_b[k])).astype(jnp.bfloat16)
        go(acc.at[q], in_y.at[k], 4, k, at.yn)
    total = None
    for k in order:
        arrived(in_x.at[k], 3, k)
        arrived(in_y.at[k], 4, k)
        plane = f32(acc[chunk(at.plane(k), at.y, at.x)]) + f32(in_x[k]) + f32(in_y[k])
        if k:
            out_z[k] = plane.astype(jnp.bfloat16)
            go(out_z.at[k], in_z.at[k], 5, k, at.zn(k))
        else:
            total = plane
    for k in at.near:
        arrived(in_z.at[k], 5, k)
        total = total + f32(in_z[k])
    for copy in started:
        copy.wait_send()
    return total


def middle_kernel(n, part_ref, own_ref, full_ref, next_ref, *scratch):
    at = Place(n)
    at.greet()
    total = sum_phase(at, part_ref, scratch[:10])
    next_ref[...] = (own_ref[...].astype(jnp.float32) + total).astype(jnp.bfloat16)
    gather_phase(at, next_ref, full_ref, *scratch[10:])


def last_kernel(n, part_ref, own_ref, next_ref, *scratch):
    at = Place(n)
    at.greet()
    total = sum_phase(at, part_ref, scratch)
    next_ref[...] = (own_ref[...].astype(jnp.float32) + total).astype(jnp.bfloat16)


def comm_call(kernel, n, collective_id, out_shape, scratch_shapes, *operands):
    vmem = pl.BlockSpec(memory_space=pltpu.VMEM)
    return pl.pallas_call(
        functools.partial(kernel, n),
        out_shape=out_shape,
        in_specs=[vmem] * len(operands),
        out_specs=jax.tree.map(lambda _: vmem, out_shape),
        scratch_shapes=scratch_shapes,
        compiler_params=pltpu.CompilerParams(
            collective_id=collective_id, has_side_effects=True, vmem_limit_bytes=40 << 20
        ),
    )(*operands)


def gather_scratch(n):
    return [
        pltpu.SemaphoreType.DMA((gather_sends(n),)),
        pltpu.SemaphoreType.DMA((n,)),
        pltpu.SemaphoreType.DMA((n,)),
    ]


def lanes(v, times):
    return jnp.concatenate([v] * times, axis=1)


def project_kernel(x_ref, gain_ref, *refs):
    weights, (out_ref, acc, squares) = refs[:6], refs[6:]
    step, last = pl.program_id(0), pl.num_programs(0) - 1
    width = x_ref.shape[2]
    wide = x_ref[...].astype(jnp.float32).reshape(-1, width)
    scaled = (wide * gain_ref[...]).astype(jnp.bfloat16)
    joined = jnp.concatenate([w[0, 0] for w in weights], axis=0)
    part = lax.dot_general(
        scaled, joined, (((1,), (1,)), ((), ())), preferred_element_type=jnp.float32
    )
    square = wide * wide
    folded = square[:, :128]
    for at in range(128, width, 128):
        folded = folded + square[:, at : at + 128]

    @pl.when(step == 0)
    def _():
        acc[...] = part
        squares[...] = folded

    @pl.when(step > 0)
    def _():
        acc[...] += part
        squares[...] += folded

    @pl.when(step == last)
    def _():
        mean = jnp.sum(squares[...], axis=1, keepdims=True) / (width * (last + 1))
        out_ref[...] = acc[...] * lax.rsqrt(mean + RMS_EPS)


def project(full, gain, weights, layer):
    n, rows, columns = full.shape
    head = weights[0].shape[2]
    chunk = columns // 8
    return pl.pallas_call(
        project_kernel,
        grid=(columns // chunk,),
        in_specs=[
            pl.BlockSpec((n, rows, chunk), lambda i: (0, 0, i)),
            pl.BlockSpec((1, chunk), lambda i: (0, i)),
        ]
        + [pl.BlockSpec((1, 1, head, chunk), lambda i: (layer, 0, 0, i))] * 6,
        out_specs=pl.BlockSpec((n * rows, 6 * head), lambda i: (0, 0)),
        out_shape=jax.ShapeDtypeStruct((n * rows, 6 * head), jnp.float32),
        scratch_shapes=[
            pltpu.VMEM((n * rows, 6 * head), jnp.float32),
            pltpu.VMEM((n * rows, 128), jnp.float32),
        ],
        compiler_params=pltpu.CompilerParams(vmem_limit_bytes=32 << 20),
    )(full, gain[layer][None], *weights)


def state_kernel(proj_ref, state_ref, table_ref, w_ref, spread_ref, *refs):
    part_ref, new_ref = refs[-2:]
    head = table_ref.shape[1]
    rows, flat = state_ref.shape[2:]
    chunk = 8 * head
    r, k, v, p, q, g = [proj_ref[:, i * head : (i + 1) * head] for i in range(6)]
    decay = jnp.exp(-jax.nn.sigmoid(table_ref[0:1] + p) * jnp.exp(jnp.float32(-0.5)))
    rate = jax.nn.sigmoid(q)
    kn = k * lax.rsqrt(jnp.sum(k * k, axis=1, keepdims=True) + 1.0)
    taken, added = kn * rate, k * rate
    kn_w, u_w = lanes(kn, chunk // head), lanes(decay * r, chunk // head)
    sums = jnp.zeros((2 * rows, head), jnp.float32)
    for at in range(0, flat, chunk):
        s = state_ref[0, 0, :, at : at + chunk]
        both = jnp.concatenate([s * kn_w, s * u_w], axis=0).astype(jnp.bfloat16)
        sums += lax.dot_general(
            both,
            spread_ref[:head, at : at + chunk],
            (((1,), (1,)), ((), ())),
            preferred_element_type=jnp.float32,
        )
    removed, read = sums[:rows], sums[rows:]
    read = (
        read
        - removed * jnp.sum(taken * r, axis=1, keepdims=True)
        + v * jnp.sum(added * r, axis=1, keepdims=True)
    )
    center = jnp.mean(read, axis=1, keepdims=True)
    off = read - center
    spread = jnp.mean(off * off, axis=1, keepdims=True)
    normed = off * lax.rsqrt(spread + GROUP_EPS) * table_ref[2:3]
    own_term = jnp.sum(r * k * table_ref[1:2], axis=1, keepdims=True) * v
    o = ((normed + own_term) * jax.nn.sigmoid(g)).astype(jnp.bfloat16)

    pair = jnp.concatenate([removed, v], axis=0)
    high = pair.astype(jnp.bfloat16)
    low = (pair - high.astype(jnp.float32)).astype(jnp.bfloat16)
    pair = jnp.concatenate([high, low], axis=1)
    decay_w, taken_w, added_w = [lanes(t, chunk // head) for t in (decay, taken, added)]
    columns = w_ref.shape[3]
    for at in range(0, columns, chunk):
        part = jnp.dot(o, w_ref[0, 0, :, at : at + chunk], preferred_element_type=jnp.float32)
        part = part.reshape(part_ref.shape[:3] + (chunk,))
        part_ref[:, :, :, at : at + chunk] = part.astype(jnp.bfloat16)
    for at in range(0, flat, chunk):
        wide = jnp.dot(pair, spread_ref[:, at : at + chunk], preferred_element_type=jnp.float32)
        new_ref[0, 0, :, at : at + chunk] = (
            state_ref[0, 0, :, at : at + chunk] * decay_w
            - wide[:rows] * taken_w
            + wide[rows:] * added_w
        )


def state_step(n, tile_rows, proj, state, table, w_out, spread, layer, earlier):
    seqs, flat = state.shape[2:]
    head, columns = w_out.shape[2:]
    rows = seqs // 2
    state_spec = pl.BlockSpec((1, 1, rows, flat), lambda i: (layer, 0, i, 0))
    whole = lambda a: pl.BlockSpec(a.shape, lambda i: (0,) * a.ndim)
    operands = [proj, state, table, w_out, spread]
    in_specs = [
        pl.BlockSpec((rows, proj.shape[1]), lambda i: (i, 0)),
        state_spec,
        whole(table),
        pl.BlockSpec((1, 1, head, columns), lambda i: (layer, 0, 0, 0)),
        whole(spread),
    ]
    if earlier is not None:
        operands.append(earlier)
        in_specs.append(pl.BlockSpec(memory_space=pl.ANY))
    per = rows // tile_rows // 2
    return pl.pallas_call(
        state_kernel,
        grid=(2,),
        in_specs=in_specs,
        out_specs=(
            pl.BlockSpec((per, 2, tile_rows, columns), lambda i: (i, 0, 0, 0)),
            state_spec,
        ),
        out_shape=(
            jax.ShapeDtypeStruct((n // 2, 2, tile_rows, columns), jnp.bfloat16),
            jax.ShapeDtypeStruct(state.shape, jnp.float32),
        ),
        input_output_aliases={} if earlier is None else {5: 1},
        compiler_params=pltpu.CompilerParams(vmem_limit_bytes=48 << 20),
    )(*operands)


def on_device_fast(n, *args):
    tokens, gain, wr, wk, wv, wd, wq, wg, bias, self_w, ro_gain, w_out, state = args
    weights = [jnp.swapaxes(w, 2, 3) for w in (wr, wk, wv, wd, wq, wg)]
    own = tokens[0]
    rows, columns = own.shape
    head = wr.shape[3]
    flat = state.shape[3]
    full_shape = jax.ShapeDtypeStruct((n, rows, columns), own.dtype)
    own_shape = jax.ShapeDtypeStruct(own.shape, own.dtype)
    position = lax.axis_index("tp")
    tables = jnp.stack([bias, self_w, ro_gain], axis=1)
    tables = lax.dynamic_slice_in_dim(tables, position * head, head, 2)
    value_of = jnp.arange(flat) // head
    spread = (jnp.arange(2 * head)[:, None] % head == value_of[None]).astype(jnp.bfloat16)

    def mixer(full, layer, earlier):
        proj = project(full, gain, weights, layer)
        return state_step(
            n, rows, proj, state, tables[layer], w_out, spread, layer, earlier
        )

    full = comm_call(gather_kernel, n, 0, full_shape, gather_scratch(n), own)
    part, new_state = mixer(full, 0, None)
    full, own = comm_call(
        middle_kernel,
        n,
        1,
        (full_shape, own_shape),
        sum_scratch(n, rows, columns) + gather_scratch(n),
        part,
        own,
    )
    part, new_state = mixer(full, 1, new_state)
    mixed = comm_call(last_kernel, n, 2, own_shape, sum_scratch(n, rows, columns), part, own)
    return mixed[None], new_state


def pick(n, *args):
    one_block = args[0].shape[2] == args[1].shape[1]
    if one_block and n % 16 == 0:
        return on_device_fast(n, *args)
    return on_device(*args)


def solution(mesh):
    return jax.shard_map(
        functools.partial(pick, mesh.shape["tp"]),
        mesh=mesh,
        in_specs=(
            P("tp", None, None),
            P(),
            P(None, "tp", None, None),
            P(None, "tp", None, None),
            P(None, "tp", None, None),
            P(None, "tp", None, None),
            P(None, "tp", None, None),
            P(None, "tp", None, None),
            P(),
            P(),
            P(),
            P(None, "tp", None, None),
            P(None, "tp", None, None),
        ),
        out_specs=(P("tp", None, None), P(None, "tp", None, None)),
        check_vma=False,
    )
```

```python
import functools

import jax
import jax.numpy as jnp
from jax import lax
from jax.experimental import pallas as pl
from jax.experimental.pallas import tpu as pltpu
from jax.sharding import PartitionSpec as P

D = 4096


RMS_EPS = 1e-06
GROUP_EPS = 0.00064


def swapped(shard, axis, stride):
    return lax.ppermute(shard, axis, [(i, i ^ 1 << stride) for i in range(lax.axis_size(axis))])


def for_sending(shard):

    def short(part):
        return part.astype(jnp.bfloat16) if part.dtype == jnp.float32 else part

    return jax.tree.map(short, shard)


def recurrent_update(
    layer_state,
    receptance_vector,
    key_vector,
    value_vector,
    decay_logits,
    learning_rate_logits,
    gate_logits,
    decay_constant,
    self_term_scale,
    head_gain_slice,
):
    highest = lax.Precision.HIGHEST
    shrink = jnp.exp(-jnp.exp(-jax.nn.softplus(-(decay_constant + decay_logits)) - 0.5))
    rate = jax.nn.sigmoid(learning_rate_logits)
    normed = key_vector * lax.rsqrt(jnp.sum(key_vector * key_vector, -1, keepdims=True) + 1.0)
    removed = jnp.einsum("...ij,...j->...i", layer_state, normed, precision=highest)
    layer_state = (
        layer_state * shrink[..., None, :]
        - removed[..., :, None] * (normed * rate)[..., None, :]
        + value_vector[..., :, None] * (key_vector * rate)[..., None, :]
    )
    readout = jnp.einsum("...ij,...j->...i", layer_state, receptance_vector, precision=highest)
    center = jnp.mean(readout, -1, keepdims=True)
    spread = jnp.mean(jnp.square(readout - center), -1, keepdims=True)
    normed_output = (readout - center) * lax.rsqrt(spread + GROUP_EPS) * head_gain_slice
    self_term = (
        jnp.sum(receptance_vector * key_vector * self_term_scale, -1, keepdims=True) * value_vector
    )
    return (
        ((normed_output + self_term) * jax.nn.sigmoid(gate_logits)).astype(jnp.bfloat16),
        layer_state,
    )


def double_gather(piece, position, first_bit, count, mover):
    for offset in range(count):
        which_bit = first_bit + offset
        partner = mover(piece, which_bit)
        lower_self = position >> which_bit & 1 == 0
        piece = jnp.where(
            lower_self, jnp.concatenate([piece, partner], 0), jnp.concatenate([partner, piece], 0)
        )
    return piece


def halve_sum(members, position, first_bit, count, mover):
    for offset in reversed(range(count)):
        which_bit = first_bit + offset
        upper_self = position >> which_bit & 1 == 1
        sends = tuple(
            (
                jnp.where(
                    upper_self, member[: member.shape[0] // 2], member[member.shape[0] // 2 :]
                )
                for member in members
            )
        )
        keeps = tuple(
            (
                jnp.where(
                    upper_self, member[member.shape[0] // 2 :], member[: member.shape[0] // 2]
                )
                for member in members
            )
        )
        arrived = mover(sends, which_bit)
        members = tuple((kept + got for kept, got in zip(keeps, arrived)))
    return members


def on_device(
    tokens,
    block_norm_gain,
    receptance_weight,
    key_weight,
    value_weight,
    decay_weight,
    learning_rate_weight,
    gate_weight,
    decay_bias_fixed,
    self_token_weight,
    readout_norm_gain,
    output_weight,
    state,
):
    columns_dev = tokens.shape[2]
    row_blocks = D // columns_dev
    low_bits = row_blocks.bit_length() - 1
    head_count = lax.axis_size("tp") // row_blocks
    high_bits = head_count.bit_length() - 1
    position = lax.axis_index("tp")
    head_index = position // row_blocks
    row_block = position % row_blocks
    head_size = receptance_weight.shape[3]
    seq_tile = tokens.shape[1]
    move_rows = lambda payload, which_bit: swapped(payload, "tp", which_bit)
    move_proj = lambda payload, which_bit: swapped(payload, "tp", which_bit)
    move_outs = lambda payload, which_bit: jax.tree.map(
        lambda part, own: part.astype(own.dtype),
        swapped(for_sending(payload), "tp", which_bit),
        payload,
    )
    move_split = lambda payload, which_bit: jax.tree.map(
        lambda part, own: part.astype(own.dtype),
        swapped(for_sending(payload), "tp", which_bit),
        payload,
    )

    def mixer(columns, layer_index):
        gain_cols = lax.dynamic_slice_in_dim(
            block_norm_gain[layer_index], row_block * columns_dev, columns_dev
        )
        wide = columns.astype(jnp.float32)
        scaled = (wide * gain_cols).astype(jnp.bfloat16)
        squares = jnp.sum(wide * wide, axis=1)
        weights = jnp.concatenate(
            [
                receptance_weight[layer_index, 0],
                key_weight[layer_index, 0],
                value_weight[layer_index, 0],
                decay_weight[layer_index, 0],
                learning_rate_weight[layer_index, 0],
                gate_weight[layer_index, 0],
            ],
            axis=1,
        )
        partial_value = jnp.dot(scaled, weights, preferred_element_type=jnp.float32)
        summed, total_sq = halve_sum((partial_value, squares), position, 0, low_bits, move_proj)
        projected = summed * lax.rsqrt(total_sq / D + RMS_EPS)[:, None]
        output_pieces = jnp.split(projected, 6, axis=1)

        def head_columns(table):
            return lax.dynamic_slice_in_dim(table[layer_index], head_index * head_size, head_size)

        layer_state = state[layer_index, 0].reshape(-1, head_size, head_size)
        out_tile, layer_state = recurrent_update(
            layer_state,
            *output_pieces,
            head_columns(decay_bias_fixed),
            head_columns(self_token_weight),
            head_columns(readout_norm_gain)
        )
        out_all = double_gather(out_tile, position, 0, low_bits, move_outs)
        branch = jnp.dot(out_all, output_weight[layer_index, 0], preferred_element_type=jnp.float32)
        return (branch, layer_state.reshape(layer_state.shape[0], head_size * head_size))

    columns = double_gather(tokens[0], position, low_bits, high_bits, move_rows)
    first_branch, first_memory = mixer(columns, 0)
    (tile_sum,) = halve_sum((first_branch,), position, low_bits, high_bits, move_split)
    tile_one = (tokens[0].astype(jnp.float32) + tile_sum).astype(jnp.bfloat16)
    columns = double_gather(tile_one, position, low_bits, high_bits, move_rows)
    second_branch, second_memory = mixer(columns, 1)
    (tile_sum,) = halve_sum((second_branch,), position, low_bits, high_bits, move_split)
    resid_rows = lax.dynamic_slice_in_dim(columns, head_index * seq_tile, seq_tile, 0)
    mixed = (resid_rows.astype(jnp.float32) + tile_sum).astype(jnp.bfloat16)
    new_state = jnp.stack([first_memory, second_memory])[:, None]
    return (mixed[None], new_state)


class Place:
    def __init__(self, n):
        me = lax.axis_index("tp")
        self.n, self.planes = n, n // 8
        self.me = me
        self.c = me % 2
        self.x = (me // 2) % 2
        self.y = (me // 4) % 2
        self.z = me // 8
        self.sib = me + 1 - 2 * self.c
        self.xn = me + 2 * (1 - 2 * self.x)
        self.yn = me + 4 * (1 - 2 * self.y)
        self.far = [self.planes // 2] + [k for k in range(1, self.planes) if k != self.planes // 2]
        self.near = [k for k in self.far if k != self.planes // 2] + [self.planes // 2]

    def plane(self, k):
        return (self.z + k) % self.planes

    def zn(self, k):
        return self.plane(k) * 8 + self.me % 8

    def greet(self):
        barrier = pltpu.get_barrier_semaphore()
        others = [self.sib, self.xn, self.yn] + [self.zn(k) for k in self.far]
        for other in others:
            pl.semaphore_signal(
                barrier, inc=1, device_id=(other,), device_id_type=pl.DeviceIdType.MESH
            )
        pl.semaphore_wait(barrier, len(others))


def remote(src, dst, send, recv, to):
    return pltpu.make_async_remote_copy(
        src_ref=src,
        dst_ref=dst,
        send_sem=send,
        recv_sem=recv,
        device_id=(to,),
        device_id_type=pl.DeviceIdType.MESH,
    )


def gather_sends(n):
    planes = n // 8
    return (planes - 1) + 3 * planes + 4 * planes + 2 * planes


def gather_phase(at, own_ref, full_ref, send, recv_a, recv_b):
    half = own_ref.shape[1] // 2
    first, second = pl.ds(0, half), pl.ds(half, half)
    started = []

    def tile(p, y, x, c):
        return ((p * 2 + y) * 2 + x) * 2 + c

    def go(src, t, to, cols=None, recv=recv_a):
        dst = full_ref.at[t]
        if cols is not None:
            src, dst = src.at[:, cols], dst.at[:, cols]
        copy = remote(src, dst, send.at[len(started)], recv.at[t], to)
        copy.start()
        started.append(copy)

    def arrived(t, cols=None, recv=recv_a):
        dst = full_ref.at[t]
        if cols is not None:
            dst = dst.at[:, cols]
        remote(dst, dst, send.at[0], recv.at[t], at.sib).wait_recv()

    for k in at.near:
        go(own_ref, at.me, at.zn(k))
    go(own_ref, at.me, at.xn)
    go(own_ref, at.me, at.yn)
    go(own_ref, at.me, at.sib)
    full_ref[at.me] = own_ref[...]

    def spread(k):
        p = at.plane(k)
        t = tile(p, at.y, 1 - at.x, at.c)
        arrived(t)
        go(full_ref.at[t], t, at.yn, first, recv_a)
        go(full_ref.at[t], t, at.sib)
        t = tile(p, 1 - at.y, at.x, at.c)
        arrived(t)
        go(full_ref.at[t], t, at.xn, second, recv_b)
        go(full_ref.at[t], t, at.sib)

    def corner(k):
        t = tile(at.plane(k), 1 - at.y, 1 - at.x, at.c)
        arrived(t, first, recv_a)
        go(full_ref.at[t], t, at.sib, first, recv_a)
        arrived(t, second, recv_b)
        go(full_ref.at[t], t, at.sib, second, recv_b)

    order = [0] + at.near
    for step, k in enumerate(order):
        if step:
            t = at.zn(k)
            arrived(t)
            go(full_ref.at[t], t, at.xn)
            go(full_ref.at[t], t, at.yn)
            go(full_ref.at[t], t, at.sib)
        if step >= 1:
            spread(order[step - 1])
        if step >= 2:
            corner(order[step - 2])
    spread(order[-1])
    if len(order) > 1:
        corner(order[-2])
    corner(order[-1])
    for k in order:
        p = at.plane(k)
        for y in (at.y, 1 - at.y):
            for x in (at.x, 1 - at.x):
                t = tile(p, y, x, 1 - at.c)
                if y is not at.y and x is not at.x:
                    arrived(t, first, recv_a)
                    arrived(t, second, recv_b)
                else:
                    arrived(t)
    for copy in started:
        copy.wait_send()


def start_loads(layer, weights, joined_ref, load):
    head = weights[0].shape[2]
    loads = [
        pltpu.make_async_copy(w.at[layer, 0], joined_ref.at[pl.ds(i * head, head)], load.at[i])
        for i, w in enumerate(weights)
    ]
    for copy in loads:
        copy.start()
    return loads


def project_rows(layer, x_ref, gain_ref, w_ref, out_ref):
    columns = x_ref.shape[2]
    chunk = columns // 8
    acc, squares = None, None
    for at in range(0, columns, chunk):
        wide = x_ref[:, :, at : at + chunk].astype(jnp.float32).reshape(-1, chunk)
        scaled = (wide * gain_ref[layer : layer + 1, at : at + chunk]).astype(jnp.bfloat16)
        part = lax.dot_general(
            scaled,
            w_ref[:, at : at + chunk],
            (((1,), (1,)), ((), ())),
            preferred_element_type=jnp.float32,
        )
        square = wide * wide
        folded = square[:, :128]
        for lane in range(128, chunk, 128):
            folded = folded + square[:, lane : lane + 128]
        acc = part if acc is None else acc + part
        squares = folded if squares is None else squares + folded
    mean = jnp.sum(squares, axis=1, keepdims=True) / columns
    out_ref[...] = acc * lax.rsqrt(mean + RMS_EPS)


def gather_kernel(n, own_ref, gain_ref, *refs, layer):
    weights, (proj_ref, full_ref, joined_ref, load, *sems) = refs[:6], refs[6:]
    loads = start_loads(layer, weights, joined_ref, load)
    at = Place(n)
    at.greet()
    gather_phase(at, own_ref, full_ref, *sems)
    for copy in loads:
        copy.wait()
    project_rows(layer, full_ref, gain_ref, joined_ref, proj_ref)


def sum_scratch(n, rows, columns):
    planes, half = n // 8, columns // 2
    tiles = lambda count, width: pltpu.VMEM((count, rows, width), jnp.bfloat16)
    return [
        tiles(n // 2, columns),
        tiles(n // 2, columns),
        tiles(planes, half),
        tiles(planes, half),
        tiles(planes, columns),
        tiles(planes, columns),
        tiles(planes, columns),
        tiles(planes, columns),
        pltpu.SemaphoreType.DMA((6 * planes,)),
        pltpu.SemaphoreType.DMA((6 * planes,)),
    ]


def sum_phase(at, part_ref, scratch):
    sib, acc, in_a, in_b, in_x, in_y, out_z, in_z, send, recv = scratch
    planes = at.planes
    half = part_ref.shape[3] // 2
    first, second = pl.ds(0, half), pl.ds(half, half)
    order = at.far + [0]
    started = []

    def go(src, dst, kind, k, to):
        copy = remote(src, dst, send.at[kind * planes + k], recv.at[kind * planes + k], to)
        copy.start()
        started.append(copy)

    def arrived(dst, kind, k):
        slot = kind * planes + k
        remote(dst, dst, send.at[slot], recv.at[slot], at.sib).wait_recv()

    def f32(v):
        return v.astype(jnp.float32)

    def chunk(p, y, x):
        return (p * 2 + y) * 2 + x

    for k in order:
        block = pl.ds(at.plane(k) * 4, 4)
        go(part_ref.at[block, 1 - at.c], sib.at[block], 0, k, at.sib)
    for k in order:
        p = at.plane(k)
        block = pl.ds(p * 4, 4)
        arrived(sib.at[block], 0, k)
        for y, x in ((1 - at.y, 1 - at.x), (at.y, 1 - at.x), (1 - at.y, at.x), (at.y, at.x)):
            q = chunk(p, y, x)
            acc[q] = (f32(part_ref[q, at.c]) + f32(sib[q])).astype(jnp.bfloat16)
            if y is not at.y and x is not at.x:
                go(acc.at[q, :, first], in_a.at[k], 1, k, at.yn)
                go(acc.at[q, :, second], in_b.at[k], 2, k, at.xn)
    for k in order:
        p = at.plane(k)
        q = chunk(p, at.y, 1 - at.x)
        arrived(in_a.at[k], 1, k)
        acc[q, :, first] = (f32(acc[q, :, first]) + f32(in_a[k])).astype(jnp.bfloat16)
        go(acc.at[q], in_x.at[k], 3, k, at.xn)
        q = chunk(p, 1 - at.y, at.x)
        arrived(in_b.at[k], 2, k)
        acc[q, :, second] = (f32(acc[q, :, second]) + f32(in_b[k])).astype(jnp.bfloat16)
        go(acc.at[q], in_y.at[k], 4, k, at.yn)
    total = None
    for k in order:
        arrived(in_x.at[k], 3, k)
        arrived(in_y.at[k], 4, k)
        plane = f32(acc[chunk(at.plane(k), at.y, at.x)]) + f32(in_x[k]) + f32(in_y[k])
        if k:
            out_z[k] = plane.astype(jnp.bfloat16)
            go(out_z.at[k], in_z.at[k], 5, k, at.zn(k))
        else:
            total = plane
    for k in at.near:
        arrived(in_z.at[k], 5, k)
        total = total + f32(in_z[k])
    for copy in started:
        copy.wait_send()
    return total


def middle_kernel(n, part_ref, own_ref, gain_ref, *refs, layer):
    weights, (proj_ref, next_ref, full_ref, joined_ref, load, *rest) = refs[:6], refs[6:]
    loads = start_loads(layer, weights, joined_ref, load)
    at = Place(n)
    at.greet()
    total = sum_phase(at, part_ref, rest[3:])
    next_ref[...] = (own_ref[...].astype(jnp.float32) + total).astype(jnp.bfloat16)
    gather_phase(at, next_ref, full_ref, *rest[:3])
    for copy in loads:
        copy.wait()
    project_rows(layer, full_ref, gain_ref, joined_ref, proj_ref)


def last_kernel(n, part_ref, own_ref, next_ref, *scratch):
    at = Place(n)
    at.greet()
    total = sum_phase(at, part_ref, scratch)
    next_ref[...] = (own_ref[...].astype(jnp.float32) + total).astype(jnp.bfloat16)


def comm_call(kernel, n, collective_id, out_shape, scratch_shapes, *operands):
    vmem, hbm = [pl.BlockSpec(memory_space=m) for m in (pltpu.VMEM, pltpu.HBM)]
    return pl.pallas_call(
        functools.partial(kernel, n),
        out_shape=out_shape,
        in_specs=[hbm if o.ndim == 4 and o.shape[0] != n // 2 else vmem for o in operands],
        out_specs=jax.tree.map(lambda _: vmem, out_shape),
        scratch_shapes=scratch_shapes,
        compiler_params=pltpu.CompilerParams(
            collective_id=collective_id, has_side_effects=True, vmem_limit_bytes=(14 if collective_id == 2 else 58) << 20
        ),
        cost_estimate=pl.CostEstimate(flops=0, bytes_accessed=50 << 20, transcendentals=0),
    )(*operands)


def gather_scratch(n):
    return [
        pltpu.SemaphoreType.DMA((gather_sends(n),)),
        pltpu.SemaphoreType.DMA((n,)),
        pltpu.SemaphoreType.DMA((n,)),
    ]


def lanes(v, times):
    return jnp.concatenate([v] * times, axis=1)


def own_head(ref, layer, head):
    position = lax.axis_index("tp")
    start = pl.multiple_of(position // 2 * (2 * head), 2 * head)
    pair = ref[layer : layer + 1, pl.ds(start, 2 * head)]
    return jnp.where(position % 2 == 0, pair[:, :head], pair[:, head:])


def state_kernel(
    layer, proj_ref, state_ref, bias_ref, self_ref, gain_ref, w_ref, spread_ref, *refs
):
    part_ref, new_ref = refs[-2:]
    head = w_ref.shape[2]
    bias, self_w, ro_gain = [own_head(t, layer, head) for t in (bias_ref, self_ref, gain_ref)]
    rows, flat = state_ref.shape[2:]
    chunk = 8 * head
    r, k, v, p, q, g = [proj_ref[:, i * head : (i + 1) * head] for i in range(6)]
    decay = jnp.exp(-jax.nn.sigmoid(bias + p) * jnp.exp(jnp.float32(-0.5)))
    rate = jax.nn.sigmoid(q)
    kn = k * lax.rsqrt(jnp.sum(k * k, axis=1, keepdims=True) + 1.0)
    taken, added = kn * rate, k * rate
    kn_w, u_w = lanes(kn, chunk // head), lanes(decay * r, chunk // head)
    sums = jnp.zeros((2 * rows, head), jnp.float32)
    for at in range(0, flat, chunk):
        s = state_ref[0, 0, :, at : at + chunk]
        both = jnp.concatenate([s * kn_w, s * u_w], axis=0).astype(jnp.bfloat16)
        sums += lax.dot_general(
            both,
            spread_ref[:head, at : at + chunk],
            (((1,), (1,)), ((), ())),
            preferred_element_type=jnp.float32,
        )
    removed, read = sums[:rows], sums[rows:]
    read = (
        read
        - removed * jnp.sum(taken * r, axis=1, keepdims=True)
        + v * jnp.sum(added * r, axis=1, keepdims=True)
    )
    center = jnp.mean(read, axis=1, keepdims=True)
    off = read - center
    spread = jnp.mean(off * off, axis=1, keepdims=True)
    normed = off * lax.rsqrt(spread + GROUP_EPS) * ro_gain
    own_term = jnp.sum(r * k * self_w, axis=1, keepdims=True) * v
    o = ((normed + own_term) * jax.nn.sigmoid(g)).astype(jnp.bfloat16)

    pair = jnp.concatenate([removed, v], axis=0)
    high = pair.astype(jnp.bfloat16)
    low = (pair - high.astype(jnp.float32)).astype(jnp.bfloat16)
    pair = jnp.concatenate([high, low], axis=1)
    decay_w, taken_w, added_w = [lanes(t, chunk // head) for t in (decay, taken, added)]
    columns = w_ref.shape[3]
    for at in range(0, columns, chunk):
        part = jnp.dot(o, w_ref[0, 0, :, at : at + chunk], preferred_element_type=jnp.float32)
        part = part.reshape(part_ref.shape[:3] + (chunk,))
        part_ref[:, :, :, at : at + chunk] = part.astype(jnp.bfloat16)
    for at in range(0, flat, chunk):
        wide = jnp.dot(pair, spread_ref[:, at : at + chunk], preferred_element_type=jnp.float32)
        new_ref[0, 0, :, at : at + chunk] = (
            state_ref[0, 0, :, at : at + chunk] * decay_w
            - wide[:rows] * taken_w
            + wide[rows:] * added_w
        )


def state_step(n, tile_rows, proj, state, tables, w_out, spread, layer, earlier):
    seqs, flat = state.shape[2:]
    head, columns = w_out.shape[2:]
    rows = seqs // 2
    state_spec = pl.BlockSpec((1, 1, rows, flat), lambda i: (layer, 0, i, 0))
    whole = lambda a: pl.BlockSpec(a.shape, lambda i: (0,) * a.ndim)
    operands = [proj, state, *tables, w_out, spread]
    in_specs = [
        pl.BlockSpec((rows, proj.shape[1]), lambda i: (i, 0)),
        state_spec,
        *[whole(t) for t in tables],
        pl.BlockSpec((1, 1, head, columns), lambda i: (layer, 0, 0, 0)),
        whole(spread),
    ]
    if earlier is not None:
        operands.append(earlier)
        in_specs.append(pl.BlockSpec(memory_space=pl.ANY))
    per = rows // tile_rows // 2
    return pl.pallas_call(
        functools.partial(state_kernel, layer),
        grid=(2,),
        in_specs=in_specs,
        out_specs=(
            pl.BlockSpec((per, 2, tile_rows, columns), lambda i: (i, 0, 0, 0)),
            state_spec,
        ),
        out_shape=(
            jax.ShapeDtypeStruct((n // 2, 2, tile_rows, columns), jnp.bfloat16),
            jax.ShapeDtypeStruct(state.shape, jnp.float32),
        ),
        input_output_aliases={} if earlier is None else {7: 1},
        compiler_params=pltpu.CompilerParams(vmem_limit_bytes=48 << 20),
    )(*operands)


def on_device_fast(n, *args):
    tokens, gain, wr, wk, wv, wd, wq, wg, bias, self_w, ro_gain, w_out, state = args
    weights = [jnp.swapaxes(w, 2, 3) for w in (wr, wk, wv, wd, wq, wg)]
    own = tokens[0]
    rows, columns = own.shape
    head = wr.shape[3]
    flat = state.shape[3]
    proj_shape = jax.ShapeDtypeStruct((n * rows, 6 * head), jnp.float32)
    gather_space = [
        pltpu.VMEM((n, rows, columns), own.dtype),
        pltpu.VMEM((6 * head, columns), wr.dtype),
        pltpu.SemaphoreType.DMA((6,)),
    ] + gather_scratch(n)
    own_shape = jax.ShapeDtypeStruct(own.shape, own.dtype)
    tables = (bias, self_w, ro_gain)
    value_of = jnp.arange(flat) // head
    spread = (jnp.arange(2 * head)[:, None] % head == value_of[None]).astype(jnp.bfloat16)

    def mixer(proj, layer, earlier):
        return state_step(n, rows, proj, state, tables, w_out, spread, layer, earlier)

    first = functools.partial(gather_kernel, layer=0)
    proj = comm_call(first, n, 0, proj_shape, gather_space, own, gain, *weights)
    part, new_state = mixer(proj, 0, None)
    proj, own = comm_call(
        functools.partial(middle_kernel, layer=1),
        n,
        1,
        (proj_shape, own_shape),
        gather_space + sum_scratch(n, rows, columns),
        part,
        own,
        gain,
        *weights,
    )
    part, new_state = mixer(proj, 1, new_state)
    mixed = comm_call(last_kernel, n, 2, own_shape, sum_scratch(n, rows, columns), part, own)
    return mixed[None], new_state


def pick(n, *args):
    one_block = args[0].shape[2] == args[1].shape[1]
    if one_block and n % 16 == 0 and 2 * args[2].shape[3] % 128 == 0:
        return on_device_fast(n, *args)
    return on_device(*args)


def solution(mesh):
    return jax.shard_map(
        functools.partial(pick, mesh.shape["tp"]),
        mesh=mesh,
        in_specs=(
            P("tp", None, None),
            P(),
            P(None, "tp", None, None),
            P(None, "tp", None, None),
            P(None, "tp", None, None),
            P(None, "tp", None, None),
            P(None, "tp", None, None),
            P(None, "tp", None, None),
            P(),
            P(),
            P(),
            P(None, "tp", None, None),
            P(None, "tp", None, None),
        ),
        out_specs=(P("tp", None, None), P(None, "tp", None, None)),
        check_vma=False,
    )
```
